32 devices in a mesh: grp: 2 (over x), ep: 16 (over z, y, core).
Axes of the slice: x: 2, y: 2, z: 4, core: 2. Of those that a mesh axis runs over, the one named last changes fastest.
Arguments:
- hidden_in: bfloat16 [512, 2048], P(('grp', 'ep')), parts along dimension 0, may hold values from -6 to 6
- state_in: float32 [512, 64, 1024], P(('grp', 'ep')), parts along dimension 0, may hold values from -3 to 3
- norm_gain: float32 [2048], replicated, may hold values from 0.1 to 1.9
- w_recept: bfloat16 [2048, 1024], P(None, 'ep'), may hold values from -0.125 to 0.125
- w_key: bfloat16 [2048, 1024], P(None, 'ep'), may hold values from -0.125 to 0.125
- w_value: bfloat16 [2048, 1024], P(None, 'ep'), may hold values from -0.125 to 0.125
- decay_base: float32 [1024], replicated, may hold values from -4 to 2
- w_decay_down: bfloat16 [2048, 128], replicated, may hold values from -0.125 to 0.125
- w_decay_up: bfloat16 [128, 1024], replicated, may hold values from -0.5 to 0.5
- w_remove_down: bfloat16 [2048, 128], replicated, may hold values from -0.125 to 0.125
- w_remove_up: bfloat16 [128, 1024], replicated, may hold values from -1 to 1
- group_gain: float32 [1024], replicated, may hold values from 0.1 to 1.9
- w_out: bfloat16 [1024, 2048], replicated, may hold values from -0.1875 to 0.1875
- ffn_gain: float32 [2048], replicated, may hold values from 0.1 to 1.9
- routes: int32 [512, 2], P(('grp', 'ep')), parts along dimension 0, may hold values from 0 to 3, all different within a row; in each aligned block of 16 rows (0 to 15, 16 to 31, ...) at most 16 rows name the same one
- route_gate: float32 [512, 2], P(('grp', 'ep')), parts along dimension 0, may hold values from 0.1 to 1
- w_gate: bfloat16 [2048, 11264], P(None, 'ep'), may hold values from -0.125 to 0.125
- w_up: bfloat16 [2048, 11264], P(None, 'ep'), may hold values from -0.125 to 0.125
- w_down: bfloat16 [11264, 2048], P('ep'), may hold values from -0.109375 to 0.109375
Outputs:
- mixed_out: bfloat16 [512, 2048], P(('grp', 'ep')), parts along dimension 0
- state_out: float32 [512, 64, 1024], P(('grp', 'ep')), parts along dimension 0
The draws below stay inside these ranges and needn't reach their ends.
There are 2 independent parts, one for each index of `grp`. The reference program is written for one: setup_inputs(seed, part) draws one part's arguments, and reference() takes and returns one part's arrays. A program takes and returns all parts, laid end to end along the dimension named above; an argument that names none is the same for every part. Nothing has to cross between parts.
Inputs may be any that keep to these rules, and one draw needn't show every extreme that they name: `routes`: each row names 2 different experts; in each aligned block of 16 rows (the rows of one device) no expert is named more than 16 times.
All inputs are finite; a program needn't handle non-finite values.
Results may differ from the reference program's by a relative error of at most 0.015.
Values may be sent and summed in bfloat16 or wider, within the bound.
A program may use at most 128 MiB of HBM per device.

```python
import math
import jax
import jax.numpy as jnp
import numpy as np
from jax import lax

D = 2048
HS = 64
RANK = 128
EXP_FF = 2816
EXP_SPLIT = 4
TOPK = 2
S_DEV = 16
INNER = 1024
SEQS = 256
EXPERTS = 4
CAP = 16
N_EP = 16


def steps_of(stream_key, extent, shards, smallest, high):
    def one(axis_at, shards_of):
        draws = jax.random.uniform(jax.random.fold_in(jax.random.fold_in(stream_key, 6), axis_at), (shards_of,), jnp.float32, smallest / len(shards), high / len(shards))
        return jnp.repeat(jnp.exp(draws), extent[axis_at] // shards_of).reshape((-1,) + (1,) * (len(extent) - axis_at - 1))

    level = one(*shards[0])
    for cut in shards[1:]:
        level = level * one(*cut)
    return level


def deal_out(rng, own, number, rows, number_of, top, most, lean):
    sequence = jax.random.permutation(rng, number_of)
    heavy_load, ordinary = shares(number_of, rows * top, most, lean, True), shares(number_of, rows * top, most, lean, False)
    places = jnp.arange(number_of)

    def named(sizes, rotation):
        used = int((sizes > 0).sum())
        fixed = max(1, used // 4)
        passed = fixed + (places - fixed + rotation * (used - fixed)) % max(1, number_of - fixed)
        return jnp.zeros((number_of,), jnp.int32).at[sequence[jnp.where(places < fixed, places, passed)]].set(jnp.asarray(sizes, jnp.int32))

    sizes = jnp.where(number % 4 == 0, named(heavy_load, number // 4), named(ordinary, number - number // 4 - 1))
    mixed = jax.random.permutation(jax.random.fold_in(own, 3), number_of)
    source_of, sink = mixed[0:number_of // 2 * 2:2], mixed[1:number_of // 2 * 2:2]
    margin = jnp.minimum(sizes[source_of] - 1, most - sizes[sink]) // 2
    margin = jnp.where((source_of == sequence[0]) | (sink == sequence[0]) | (sizes[sink] == 0), 0, jnp.maximum(margin, 0))
    passed = jax.random.randint(jax.random.fold_in(own, 4), (number_of // 2,), 0, 1 << 20) % (margin + 1)
    sizes = sizes.at[source_of].add(-passed).at[sink].add(passed)
    members = jnp.searchsorted(jnp.cumsum(sizes), jnp.arange(rows * top), side="right").astype(jnp.int32)
    listing = members.reshape(top, rows).T
    listing = listing[jax.random.permutation(jax.random.fold_in(own, 1), rows)]
    rotation = jax.random.randint(jax.random.fold_in(own, 2), (rows, 1), 0, top)
    return jnp.take_along_axis(listing, (jnp.arange(top)[None, :] + rotation) % top, axis=1)


def shares(number_of, total, limit, slope, full):
    portions = [(1 << 20) // math.isqrt(standing ** slope) + 1 for standing in range(1, number_of + 1)]
    largest = limit if full else min(limit, max(-(-total // number_of), total * portions[0] // sum(portions)))
    least = 1 if total - largest >= number_of - 1 else 0
    holding, surplus = [largest] + [least] * (number_of - 1), total - largest - least * (number_of - 1)
    while surplus > 0:
        free = [i for i in range(1, number_of) if holding[i] < largest] or [i for i in range(1, number_of) if holding[i] < limit]
        whole, left = sum([portions[i] for i in free]), surplus
        for i in free:
            extra = min(limit - holding[i], max(1, left * portions[i] // whole), surplus)
            holding[i] = holding[i] + extra
            surplus = surplus - extra
    return np.array(holding)


def bell_draw(key, extent, scale, most, cuts=(), kind=jnp.bfloat16):
    gain = steps_of(key, extent, cuts, -0.22, 0.18) if cuts else 1.0
    entries = jax.random.normal(key, extent, jnp.float32) * scale * gain
    return jnp.minimum(jnp.maximum(entries, -most), most).astype(kind)


def setup_inputs(seed: int = 0, part: int = 0) -> dict:
    splits = jax.random.split(jax.random.key(seed), 20)
    own_keys = jax.random.split(jax.random.fold_in(splits[19], part), 20)
    hidden_in = bell_draw(own_keys[0], (SEQS, D), 1.0, 6.0, ((0, 16),))
    state_in = bell_draw(own_keys[1], (SEQS, HS, INNER), 0.5, 3.0, ((0, 16),), jnp.float32)
    norm_gain = jnp.clip(1.0 + 0.18 * jax.random.normal(splits[2], (D,), jnp.float32), 0.1, 1.9)
    w_recept = bell_draw(splits[3], (D, INNER), D ** -0.5, 0.125, ((1, 16),))
    w_key = bell_draw(splits[4], (D, INNER), D ** -0.5, 0.125, ((1, 16),))
    w_value = bell_draw(splits[5], (D, INNER), D ** -0.5, 0.125, ((1, 16),))
    decay_base = jnp.clip(jax.random.uniform(splits[6], (INNER,), jnp.float32, -4.0, 2.0), -4.0, 2.0)
    w_decay_down = bell_draw(splits[7], (D, RANK), D ** -0.5, 0.125)
    w_decay_up = bell_draw(splits[8], (RANK, INNER), RANK ** -0.5, 0.5)
    w_remove_down = bell_draw(splits[9], (D, RANK), D ** -0.5, 0.125)
    w_remove_up = bell_draw(splits[10], (RANK, INNER), (RANK // 4) ** -0.5, 1.0)
    group_gain = jnp.clip(1.0 + 0.18 * jax.random.normal(splits[11], (INNER,), jnp.float32), 0.1, 1.9)
    w_out = bell_draw(splits[12], (INNER, D), INNER ** -0.5, 0.1875)
    ffn_gain = jnp.clip(1.0 + 0.18 * jax.random.normal(splits[13], (D,), jnp.float32), 0.1, 1.9)
    routes_keys = jax.random.split(jax.random.fold_in(own_keys[14], 1), SEQS // S_DEV)
    routes_turns = jax.random.permutation(jax.random.fold_in(own_keys[14], 3), SEQS // S_DEV)
    routes = jax.vmap(lambda own, number: deal_out(jax.random.fold_in(own_keys[14], 2), own, number, S_DEV, EXPERTS, TOPK, CAP, 2))(routes_keys, routes_turns).reshape((SEQS, TOPK))
    route_gate = jnp.clip(0.1 + 0.9 * jax.random.uniform(own_keys[15], (SEQS, TOPK), jnp.float32) ** steps_of(own_keys[15], (SEQS, TOPK), ((0, 16),), -0.2, 0.2), 0.1, 1.0)
    w_gate = bell_draw(splits[16], (D, EXPERTS * EXP_FF), D ** -0.5, 0.125, ((1, 16),))
    w_up = bell_draw(splits[17], (D, EXPERTS * EXP_FF), D ** -0.5, 0.125, ((1, 16),))
    w_down = bell_draw(splits[18], (EXPERTS * EXP_FF, D), EXP_FF ** -0.5, 0.109375, ((0, 16),))
    return {"hidden_in": hidden_in, "state_in": state_in, "norm_gain": norm_gain, "w_recept": w_recept, "w_key": w_key, "w_value": w_value, "decay_base": decay_base, "w_decay_down": w_decay_down, "w_decay_up": w_decay_up, "w_remove_down": w_remove_down, "w_remove_up": w_remove_up, "group_gain": group_gain, "w_out": w_out, "ffn_gain": ffn_gain, "routes": routes, "route_gate": route_gate, "w_gate": w_gate, "w_up": w_up, "w_down": w_down}


norm_eps = 1e-06
group_eps = 0.00064

def scaled_rows(values, scale_gain):
    floats = values.astype(jnp.float32)
    return floats * lax.rsqrt(lax.optimization_barrier(jnp.mean(floats * floats, axis=-1, keepdims=True)) + norm_eps) * scale_gain

def update_state(state_in, receptance, new_keys, new_values, decay_rate, removal):
    seq_count = state_in.shape[0]
    head_size = state_in.shape[1]
    head_count = state_in.shape[2] // head_size
    shape_heads = (seq_count, head_count, head_size)
    recept_heads = receptance.astype(jnp.float32).reshape(shape_heads)
    key_heads = new_keys.astype(jnp.float32).reshape(shape_heads)
    value_heads = new_values.astype(jnp.float32).reshape(shape_heads)
    unit_keys = key_heads * lax.rsqrt(lax.optimization_barrier(jnp.sum(key_heads * key_heads, axis=-1, keepdims=True)) + norm_eps)
    blocks = state_in.reshape(seq_count, head_size, head_count, head_size)
    recalled = jnp.einsum('svhk,shk->svh', blocks, unit_keys, precision=lax.Precision.HIGHEST)
    removed = unit_keys * removal.reshape(shape_heads)
    updated = blocks * decay_rate.reshape(seq_count, 1, head_count, head_size) - recalled[..., None] * removed[:, None] + jnp.swapaxes(value_heads, 1, 2)[..., None] * key_heads[:, None]
    readout = jnp.einsum('svhk,shk->shv', updated, recept_heads, precision=lax.Precision.HIGHEST)
    return (updated.reshape(state_in.shape), readout)

def group_scale(readout, scale_gain):
    center = readout - lax.optimization_barrier(jnp.mean(readout, axis=-1, keepdims=True))
    spread = lax.optimization_barrier(jnp.mean(center * center, axis=-1, keepdims=True))
    normed = center * lax.rsqrt(spread + group_eps)
    return (normed.reshape(readout.shape[0], -1) * scale_gain).astype(jnp.bfloat16)

def decay_of(normed, w_decay_down, w_decay_up, decay_base):
    decay_low = jnp.dot(normed, w_decay_down, preferred_element_type=jnp.float32).astype(jnp.bfloat16)
    decay_act = jnp.tanh(decay_low.astype(jnp.float32)).astype(jnp.bfloat16)
    decay_pre = decay_base + jnp.dot(decay_act, w_decay_up, preferred_element_type=jnp.float32)
    return jnp.exp(-jnp.exp(-jax.nn.softplus(-decay_pre) - 0.5))

def removal_of(normed, w_remove_down, w_remove_up):
    remove_low = jnp.dot(normed, w_remove_down, preferred_element_type=jnp.float32).astype(jnp.bfloat16)
    return jax.nn.sigmoid(jnp.dot(remove_low, w_remove_up, preferred_element_type=jnp.float32))

def reference(hidden_in, state_in, norm_gain, w_recept, w_key, w_value, decay_base, w_decay_down, w_decay_up, w_remove_down, w_remove_up, group_gain, w_out, ffn_gain, routes, route_gate, w_gate, w_up, w_down):
    normed = scaled_rows(hidden_in, norm_gain).astype(jnp.bfloat16)
    receptance = jnp.dot(normed, w_recept, preferred_element_type=jnp.float32).astype(jnp.bfloat16)
    new_keys = jnp.dot(normed, w_key, preferred_element_type=jnp.float32).astype(jnp.bfloat16)
    new_values = jnp.dot(normed, w_value, preferred_element_type=jnp.float32).astype(jnp.bfloat16)
    decay_rate = decay_of(normed, w_decay_down, w_decay_up, decay_base)
    removal = removal_of(normed, w_remove_down, w_remove_up)
    state_out, readout = update_state(state_in, receptance, new_keys, new_values, decay_rate, removal)
    grouped = group_scale(readout, group_gain)
    residual = hidden_in.astype(jnp.float32) + jnp.dot(grouped, w_out, preferred_element_type=jnp.float32)
    expert_in = scaled_rows(residual, ffn_gain).astype(jnp.bfloat16)
    chosen = routes.reshape(N_EP, S_DEV * TOPK)
    hit_table = (chosen[..., None] == jnp.arange(EXPERTS, dtype=jnp.int32)).astype(jnp.int32)
    slot_index = lax.optimization_barrier(jnp.sum((jnp.cumsum(hit_table, axis=1) - 1) * hit_table, axis=2))
    slot_table = (slot_index[..., None] == jnp.arange(CAP, dtype=jnp.int32)).astype(jnp.float32)
    placed = hit_table.astype(jnp.float32)[..., None] * slot_table[:, :, None, :]
    placed = placed.reshape(N_EP, S_DEV, TOPK, EXPERTS, CAP)
    dispatch = lax.optimization_barrier(jnp.sum(placed, axis=2))
    combine = lax.optimization_barrier(jnp.sum(placed * route_gate.reshape(N_EP, S_DEV, TOPK)[..., None, None], axis=2))
    blocks_in = expert_in.reshape(N_EP, S_DEV, D).astype(jnp.float32)
    gathered = jnp.einsum('nsec,nsd->encd', dispatch, blocks_in, precision=lax.Precision.HIGHEST).astype(jnp.bfloat16)
    quarter = EXP_FF // EXP_SPLIT

    def run_expert(operands):
        inputs, index = operands
        flat_rows = inputs.reshape(N_EP * CAP, D)
        gate_cols = lax.dynamic_slice_in_dim(w_gate, index * EXP_FF, EXP_FF, 1)
        up_cols = lax.dynamic_slice_in_dim(w_up, index * EXP_FF, EXP_FF, 1)
        down_rows = lax.dynamic_slice_in_dim(w_down, index * EXP_FF, EXP_FF, 0)
        gate_pre = jnp.dot(flat_rows, gate_cols, preferred_element_type=jnp.float32)
        up_pre = jnp.dot(flat_rows, up_cols, preferred_element_type=jnp.float32)
        hidden = (jax.nn.silu(gate_pre) * up_pre).astype(jnp.bfloat16)
        parts = jnp.einsum('rqf,qfd->qrd', hidden.reshape(N_EP * CAP, EXP_SPLIT, quarter).astype(jnp.float32), down_rows.reshape(EXP_SPLIT, quarter, D).astype(jnp.float32))
        rounded = lax.optimization_barrier(parts.astype(jnp.bfloat16))
        return lax.optimization_barrier(jnp.sum(rounded.astype(jnp.float32), axis=0)).reshape(N_EP, CAP, D)
    outputs = lax.map(run_expert, (gathered, jnp.arange(EXPERTS, dtype=jnp.int32)))
    routed = jnp.einsum('nsec,encd->nsd', combine, outputs, precision=lax.Precision.HIGHEST).reshape(N_EP * S_DEV, D)
    mixed_out = (residual + routed).astype(jnp.bfloat16)
    return (mixed_out, state_out)
```

```python
import functools

import jax
import jax.numpy as jnp
from jax import lax
from jax.experimental import pallas as pl
from jax.experimental.pallas import tpu as pltpu
from jax.sharding import PartitionSpec as P

EXP_SPLIT = 4
MESH = pl.DeviceIdType.MESH
F32 = jnp.float32
BF16 = jnp.bfloat16

norm_eps = 1e-06
group_eps = 0.00064


def scaled_rows(values, scale_gain):
    floats = values.astype(F32)
    return (
        floats
        * lax.rsqrt(jnp.mean(floats * floats, axis=-1, keepdims=True) + norm_eps)
        * scale_gain
    )


def dot(lhs, rhs):
    return jnp.dot(lhs, rhs, preferred_element_type=F32)


def dot_t(lhs, rhs):
    return lax.dot_general(lhs, rhs, (((1,), (1,)), ((), ())), preferred_element_type=F32)


def split_dot(lhs, rhs):
    high = lhs.astype(BF16)
    low = (lhs - high.astype(F32)).astype(BF16)
    return dot(high, rhs) + dot(low, rhs)


def remote(src, dst, send_sem, recv_sem, device):
    return pltpu.make_async_remote_copy(
        src_ref=src,
        dst_ref=dst,
        send_sem=send_sem,
        recv_sem=recv_sem,
        device_id={"ep": device},
        device_id_type=MESH,
    )


def place(ep_size):
    me = lax.axis_index("ep")
    return me, me // 4, (me // 2) % 2, me % 2, ep_size // 4


def greet_all(me, ep_size):
    barrier = pltpu.get_barrier_semaphore()
    for step in range(1, ep_size):
        pl.semaphore_signal(
            barrier, inc=1, device_id={"ep": lax.rem(me + step, ep_size)}, device_id_type=MESH
        )
    return barrier


class Gather:
    def __init__(self, ep_size, slots, z_sems, b_sems, c_sems):
        self.me, self.a, self.b, self.c, self.planes = place(ep_size)
        self.slots = slots
        self.z, self.bs, self.cs = z_sems, b_sems, c_sems
        self.sent = []

    def slot(self, core, back, side):
        plane = lax.rem(self.a + (self.planes - back), self.planes)
        return self.slots.at[core, plane * 2 + side]

    def device(self, plane, side, core):
        return (plane * 2 + side) * 2 + core

    def along(self, i):
        ref = self.slot(self.c, 0, self.b)
        plane = lax.rem(self.a + i, self.planes)
        return remote(
            ref, ref, self.z.at[0, i], self.z.at[1, i], self.device(plane, self.b, self.c)
        )

    def across(self, i):
        ref = self.slot(self.c, i, self.b)
        return remote(
            ref, ref, self.bs.at[0, i], self.bs.at[1, i], self.device(self.a, 1 - self.b, self.c)
        )

    def to_core(self, kind, i):
        ref = self.slot(self.c, i, self.b if kind == 0 else 1 - self.b)
        return remote(
            ref,
            ref,
            self.cs.at[0, kind, i],
            self.cs.at[1, kind, i],
            self.device(self.a, self.b, 1 - self.c),
        )

    def go(self, copy):
        copy.start()
        self.sent.append(copy)

    def start(self):
        for i in reversed(range(1, self.planes)):
            self.go(self.along(i))
        self.go(self.across(0))
        self.go(self.to_core(0, 0))

    def arrived(self, ref, sem):
        remote(ref, ref, sem, sem, self.me).wait_recv()

    def relay_side(self, i):
        self.arrived(self.slot(self.c, i, 1 - self.b), self.bs.at[1, i])
        self.go(self.to_core(1, i))

    def finish(self):
        for i in range(1, self.planes):
            self.arrived(self.slot(self.c, i, self.b), self.z.at[1, i])
            self.go(self.across(i))
            self.go(self.to_core(0, i))
            self.relay_side(i - 1)
        self.relay_side(self.planes - 1)

    def finish_core(self):
        for i in range(self.planes):
            self.arrived(self.slot(1 - self.c, i, self.b), self.cs.at[1, 0, i])
            self.arrived(self.slot(1 - self.c, i, 1 - self.b), self.cs.at[1, 1, i])

    def drain(self):
        for copy in self.sent:
            copy.wait_send()


def gather_scratch(ep_size, rows, width):
    planes = ep_size // 4
    return [
        pltpu.VMEM((2, ep_size // 2, rows, width), BF16),
        pltpu.SemaphoreType.DMA((2, planes)),
        pltpu.SemaphoreType.DMA((2, planes)),
        pltpu.SemaphoreType.DMA((2, 2, planes)),
    ]


def load_all(pairs, sems):
    copies = [pltpu.make_async_copy(src, dst, sems.at[n]) for n, (src, dst) in enumerate(pairs)]
    for copy in copies:
        copy.start()
    return copies


def project_kernel(
    ep_size, experts, hidden_ref, gain_ref, base_ref, routes_ref, gates_ref,
    wr, wk, wv, wdd, wdu, wrd, wru,
    got_ref, decay_ref, removal_ref,
    wdd_v, wdu_v, wrd_v, wru_v, load_sems,
    joint, slots, z_sems, b_sems, c_sems, outbox, inbox, x_send, x_recv,
):
    me, a, b, c, planes = place(ep_size)
    rows, width = hidden_ref.shape
    part = wr.shape[0]
    lanes = joint.shape[0]
    barrier = greet_all(me, ep_size)
    loads = load_all(
        [(wdd, wdd_v), (wrd, wrd_v), (wdu, wdu_v), (wru, wru_v)]
        + [(w, joint.at[pl.ds(n * part, part)]) for n, w in enumerate((wr, wk, wv))],
        load_sems,
    )
    if lanes > 3 * part:
        joint[3 * part :, :] = jnp.zeros((lanes - 3 * part, joint.shape[1]), BF16)
    normed = scaled_rows(hidden_ref[...], gain_ref[...]).astype(BF16)
    slots[c, a * 2 + b] = normed
    pl.semaphore_wait(barrier, ep_size - 1)
    gather = Gather(ep_size, slots, z_sems, b_sems, c_sems)
    gather.start()

    for copy in loads[:4]:
        copy.wait()
    decay_low = dot(normed, wdd_v[...]).astype(BF16)
    decay_act = jnp.tanh(decay_low.astype(F32)).astype(BF16)
    decay_pre = base_ref[...] + dot(decay_act, wdu_v[...])
    decay_ref[...] = jnp.exp(-jnp.exp(-jax.nn.softplus(-decay_pre) - 0.5))
    remove_low = dot(normed, wrd_v[...]).astype(BF16)
    removal_ref[...] = jax.nn.sigmoid(dot(remove_low, wru_v[...]))
    for copy in loads[4:]:
        copy.wait()
    lane = lax.broadcasted_iota(jnp.int32, (rows, lanes), 1) - 3 * part
    weight = jnp.zeros((rows, lanes), F32)
    for j in range(routes_ref.shape[1]):
        chosen = routes_ref[:, j : j + 1]
        hit = (lane == chosen) | (lane == chosen + experts)
        weight = weight + jnp.where(hit, gates_ref[:, j : j + 1], 0.0)
    high = weight.astype(BF16).astype(F32)
    spare = jnp.where(lane < experts, high, weight - high)
    spare = jnp.where(lane >= 0, spare, 0.0)

    gather.finish()
    gather.finish_core()
    rows_all = slots[...].reshape(ep_size * rows, width)
    spread = dot_t(rows_all, joint[...]).reshape(2, ep_size // 2, rows, lanes)
    outbox[...] = (spread + spare[None, None]).astype(BF16)
    sends = []
    for step in range(1, ep_size):
        other = lax.rem(me + step, ep_size)
        copy = remote(
            outbox.at[other % 2, other // 2],
            inbox.at[c, a * 2 + b],
            x_send.at[step],
            x_recv.at[step],
            other,
        )
        copy.start()
        sends.append(copy)
    inbox[c, a * 2 + b] = outbox[c, a * 2 + b]
    for step in range(1, ep_size):
        other = lax.rem(me + (ep_size - step), ep_size)
        ref = inbox.at[other % 2, other // 2]
        remote(ref, ref, x_recv.at[step], x_recv.at[step], me).wait_recv()
    got_ref[...] = inbox[...]
    gather.drain()
    for copy in sends:
        copy.wait_send()


def mixer_kernel(
    ep_size, hidden_ref, got_ref, decay_ref, removal_ref, ggain_ref, fgain_ref, state_ref, w_out,
    state_out, residual_ref, expert_ref,
    w_out_v, load_sem, recept, keys, values, group, grouped,
):
    step = pl.program_id(0)
    seqs, head, inner = state_ref.shape
    heads = inner // head
    part = inner // ep_size
    load = pltpu.make_async_copy(w_out, w_out_v, load_sem)

    @pl.when(step == 0)
    def _():
        load.start()
        for d in range(ep_size):
            block = got_ref[d % 2, d // 2].astype(F32)
            own = slice(d * part, (d + 1) * part)
            recept[:, own] = block[:, 0:part]
            keys[:, own] = block[:, part : 2 * part]
            values[:, own] = block[:, 2 * part : 3 * part]
        group[...] = (
            lax.broadcasted_iota(jnp.int32, (inner, heads), 0) // head
            == lax.broadcasted_iota(jnp.int32, (inner, heads), 1)
        ).astype(F32).astype(BF16)

    these = pl.ds(pl.multiple_of(step * seqs, seqs), seqs)
    spread = (
        lax.broadcasted_iota(jnp.int32, (heads, inner), 1) // head
        == lax.broadcasted_iota(jnp.int32, (heads, inner), 0)
    ).astype(F32).astype(BF16)
    own_row = (
        lax.broadcasted_iota(jnp.int32, (head, inner), 1) % head
        == lax.broadcasted_iota(jnp.int32, (head, inner), 0)
    ).astype(F32)
    gather = group[...]
    key = keys[these, :]
    sums = split_dot(key * key, gather)
    unit = key * split_dot(lax.rsqrt(sums + norm_eps), spread)
    removed = unit * removal_ref[these, :]
    recept_now = recept[these, :]
    value_now = values[these, :]
    decay = decay_ref[these, :]
    out_rows = []
    for s in range(seqs):
        one = slice(s, s + 1)
        block = state_ref[s]
        recalled = split_dot(block * unit[one], gather)
        value_col = dot((own_row * value_now[one]).astype(BF16), gather)
        updated = (
            block * decay[one]
            - split_dot(recalled, spread) * removed[one]
            + dot(value_col.astype(BF16), spread) * key[one]
        )
        state_out[s] = updated
        readout = split_dot(updated * recept_now[one], gather)
        center = readout - jnp.mean(readout, axis=0, keepdims=True)
        var = jnp.mean(center * center, axis=0, keepdims=True)
        normed = center * lax.rsqrt(var + group_eps)
        out_rows.append(jnp.sum(split_dot(normed, spread) * own_row, axis=0, keepdims=True))
    grouped[these, :] = jnp.concatenate(out_rows, axis=0) * ggain_ref[...]

    @pl.when(step == pl.num_programs(0) - 1)
    def _():
        load.wait()
        residual = hidden_ref[...].astype(F32) + dot(grouped[...].astype(BF16), w_out_v[...])
        residual_ref[...] = residual
        expert_ref[...] = scaled_rows(residual, fgain_ref[...]).astype(BF16)


def expert_kernel(
    ep_size, experts, part, expert_ref, residual_ref, got_ref, wg, wu, wd,
    mixed_ref,
    wg_v, wu_v, wd_v, load_sems,
    slots, z_sems, b_sems, c_sems,
    mine, c_out, c_in, c_sem, b_out, b_in, b_sem, z_out, z_in, z_sem,
):
    me, a, b, c, planes = place(ep_size)
    rows, width = expert_ref.shape
    half = ep_size // 2
    barrier = greet_all(me, ep_size)
    loads = load_all([(wg, wg_v), (wu, wu_v), (wd, wd_v)], load_sems)
    slots[c, a * 2 + b] = expert_ref[...]
    pl.semaphore_wait(barrier, ep_size - 1)
    gather = Gather(ep_size, slots, z_sems, b_sems, c_sems)
    gather.start()
    expert = me // EXP_SPLIT
    lane = lax.broadcasted_iota(jnp.int32, got_ref.shape[2:], 1) - 3 * part
    column = (lane == expert) | (lane == expert + experts)
    for copy in loads:
        copy.wait()

    def run(core):
        flat = slots[core].reshape(half * rows, width)
        gate_pre = dot_t(flat, wg_v[...])
        up_pre = dot_t(flat, wu_v[...])
        hidden = (jax.nn.silu(gate_pre) * up_pre).astype(BF16)
        weight = jnp.sum(
            jnp.where(column[None], got_ref[core].astype(F32), 0.0), axis=-1, keepdims=True
        )
        return dot(hidden, wd_v[...]).reshape(half, rows, width) * weight

    gather.finish()
    gather.finish_core()
    sends = []
    c_out[...] = run(1 - c).astype(BF16)
    for i in range(planes):
        plane = lax.rem(a + i, planes)
        copy = remote(
            c_out.at[pl.ds(plane * 2, 2)],
            c_in.at[pl.ds(plane * 2, 2)],
            c_sem.at[0, i],
            c_sem.at[1, i],
            (a * 2 + b) * 2 + 1 - c,
        )
        copy.start()
        sends.append(copy)
    mine[...] = run(c)
    order = list(range(1, planes)) + [0]
    for i in order:
        plane = lax.rem(a + i, planes)
        both = c_in.at[pl.ds(plane * 2, 2)]
        remote(both, both, c_sem.at[1, i], c_sem.at[1, i], me).wait_recv()
        far = plane * 2 + 1 - b
        b_out[plane] = (mine[far] + c_in[far].astype(F32)).astype(BF16)
        copy = remote(
            b_out.at[plane],
            b_in.at[plane],
            b_sem.at[0, i],
            b_sem.at[1, i],
            (a * 2 + 1 - b) * 2 + c,
        )
        copy.start()
        sends.append(copy)
    total = residual_ref[...]
    for i in order:
        plane = lax.rem(a + i, planes)
        ref = b_in.at[plane]
        remote(ref, ref, b_sem.at[1, i], b_sem.at[1, i], me).wait_recv()
        near = plane * 2 + b
        joined = mine[near] + c_in[near].astype(F32) + b_in[plane].astype(F32)
        if i == 0:
            total = total + joined
        else:
            z_out[i] = joined.astype(BF16)
            copy = remote(
                z_out.at[i],
                z_in.at[i],
                z_sem.at[0, i],
                z_sem.at[1, i],
                (plane * 2 + b) * 2 + c,
            )
            copy.start()
            sends.append(copy)
    for i in range(1, planes):
        ref = z_in.at[i]
        remote(ref, ref, z_sem.at[1, i], z_sem.at[1, i], me).wait_recv()
        total = total + z_in[i].astype(F32)
    mixed_ref[...] = total.astype(BF16)
    gather.drain()
    for copy in sends:
        copy.wait_send()


VM = pl.BlockSpec(memory_space=pltpu.VMEM)
ANY = pl.BlockSpec(memory_space=pl.ANY)
HBM = pl.BlockSpec(memory_space=pltpu.HBM)


def cost(us):
    return pl.CostEstimate(flops=int(us * 2e7), bytes_accessed=2**20, transcendentals=0)


def shards(
    hidden_in, state_in, norm_gain, w_recept, w_key, w_value, decay_base, w_decay_down,
    w_decay_up, w_remove_down, w_remove_up, group_gain, w_out, ffn_gain, routes, route_gate,
    w_gate, w_up, w_down,
):
    ep_size = lax.axis_size("ep")
    experts = ep_size // EXP_SPLIT
    rows, width = hidden_in.shape
    head, inner = state_in.shape[1:]
    part = w_recept.shape[1]
    lanes = -(-(3 * part + 2 * experts) // 128) * 128
    half, planes = ep_size // 2, ep_size // 4

    def like(array):
        return pltpu.VMEM(array.shape, array.dtype)

    loaded = (w_decay_down, w_decay_up, w_remove_down, w_remove_up)
    w_gate, w_up = w_gate.T, w_up.T
    got, decay, removal = pl.pallas_call(
        functools.partial(project_kernel, ep_size, experts),
        out_shape=(
            jax.ShapeDtypeStruct((2, half, rows, lanes), BF16),
            jax.ShapeDtypeStruct((rows, inner), F32),
            jax.ShapeDtypeStruct((rows, inner), F32),
        ),
        in_specs=[VM] * 5 + [HBM] * 7,
        out_specs=(VM, VM, VM),
        scratch_shapes=[like(w) for w in loaded]
        + [pltpu.SemaphoreType.DMA((7,)), pltpu.VMEM((lanes, width), BF16)]
        + gather_scratch(ep_size, rows, width)
        + [
            pltpu.VMEM((2, half, rows, lanes), BF16),
            pltpu.VMEM((2, half, rows, lanes), BF16),
            pltpu.SemaphoreType.DMA((ep_size,)),
            pltpu.SemaphoreType.DMA((ep_size,)),
        ],
        compiler_params=pltpu.CompilerParams(
            collective_id=0, has_side_effects=True, vmem_limit_bytes=20 * 2**20
        ),
        cost_estimate=cost(20000),
        name="project",
    )(
        hidden_in, norm_gain.reshape(1, -1), decay_base.reshape(1, -1), routes, route_gate,
        w_recept.T, w_key.T, w_value.T, *loaded
    )

    seqs = min(8, rows)
    whole = lambda *shape: pl.BlockSpec(shape, lambda s: (0,) * len(shape))
    state_spec = pl.BlockSpec((seqs, head, inner), lambda s: (s, 0, 0))
    state_out, residual, expert_in = pl.pallas_call(
        functools.partial(mixer_kernel, ep_size),
        grid=(rows // seqs,),
        out_shape=(
            jax.ShapeDtypeStruct(state_in.shape, F32),
            jax.ShapeDtypeStruct((rows, width), F32),
            jax.ShapeDtypeStruct((rows, width), BF16),
        ),
        in_specs=[
            whole(rows, width),
            whole(2, half, rows, lanes),
            whole(rows, inner),
            whole(rows, inner),
            whole(1, inner),
            whole(1, width),
            state_spec,
            ANY,
        ],
        out_specs=(state_spec, whole(rows, width), whole(rows, width)),
        scratch_shapes=[
            like(w_out),
            pltpu.SemaphoreType.DMA,
            pltpu.VMEM((rows, inner), F32),
            pltpu.VMEM((rows, inner), F32),
            pltpu.VMEM((rows, inner), F32),
            pltpu.VMEM((inner, inner // head), BF16),
            pltpu.VMEM((rows, inner), F32),
        ],
        compiler_params=pltpu.CompilerParams(
            dimension_semantics=("arbitrary",), vmem_limit_bytes=32 * 2**20
        ),
        cost_estimate=cost(10000),
        name="mixer",
    )(
        hidden_in, got, decay, removal, group_gain.reshape(1, -1), ffn_gain.reshape(1, -1),
        state_in, w_out,
    )

    mixed_out = pl.pallas_call(
        functools.partial(expert_kernel, ep_size, experts, part),
        out_shape=jax.ShapeDtypeStruct((rows, width), BF16),
        in_specs=[VM] * 3 + [ANY] * 3,
        out_specs=VM,
        scratch_shapes=[like(w_gate), like(w_up), like(w_down), pltpu.SemaphoreType.DMA((3,))]
        + gather_scratch(ep_size, rows, width)
        + [
            pltpu.VMEM((half, rows, width), F32),
            pltpu.VMEM((half, rows, width), BF16),
            pltpu.VMEM((half, rows, width), BF16),
            pltpu.SemaphoreType.DMA((2, planes)),
            pltpu.VMEM((planes, rows, width), BF16),
            pltpu.VMEM((planes, rows, width), BF16),
            pltpu.SemaphoreType.DMA((2, planes)),
            pltpu.VMEM((planes, rows, width), BF16),
            pltpu.VMEM((planes, rows, width), BF16),
            pltpu.SemaphoreType.DMA((2, planes)),
        ],
        compiler_params=pltpu.CompilerParams(
            collective_id=1, has_side_effects=True, vmem_limit_bytes=48 * 2**20
        ),
        cost_estimate=cost(20000),
        name="experts",
    )(expert_in, residual, got, w_gate, w_up, w_down)
    return (mixed_out, state_out)


def solution(mesh):
    placed = (
        P(("grp", "ep"), None),
        P(("grp", "ep"), None, None),
        P(),
        P(None, "ep"),
        P(None, "ep"),
        P(None, "ep"),
        P(),
        P(),
        P(),
        P(),
        P(),
        P(),
        P(),
        P(),
        P(("grp", "ep"), None),
        P(("grp", "ep"), None),
        P(None, "ep"),
        P(None, "ep"),
        P("ep", None),
    )
    return jax.shard_map(
        shards,
        mesh=mesh,
        in_specs=placed,
        out_specs=(P(("grp", "ep"), None), P(("grp", "ep"), None, None)),
        check_vma=False,
    )
```

```python
import functools

import jax
import jax.numpy as jnp
from jax import lax
from jax.experimental import pallas as pl
from jax.experimental.pallas import tpu as pltpu
from jax.sharding import PartitionSpec as P

EXP_SPLIT = 4
MIX = 4
FULL = 67_043_328
MESH = pl.DeviceIdType.MESH
F32 = jnp.float32
BF16 = jnp.bfloat16

norm_eps = 1e-06
group_eps = 0.00064


def scaled_rows(values, scale_gain):
    floats = values.astype(F32)
    return (
        floats
        * lax.rsqrt(jnp.mean(floats * floats, axis=-1, keepdims=True) + norm_eps)
        * scale_gain
    )


def dot(lhs, rhs):
    return jnp.dot(lhs, rhs, preferred_element_type=F32)


def dot_t(lhs, rhs):
    return lax.dot_general(lhs, rhs, (((1,), (1,)), ((), ())), preferred_element_type=F32)


def split_dot(lhs, rhs):
    high = lhs.astype(BF16)
    low = (lhs - high.astype(F32)).astype(BF16)
    return dot(high, rhs) + dot(low, rhs)


def remote(src, dst, send_sem, recv_sem, device):
    return pltpu.make_async_remote_copy(
        src_ref=src,
        dst_ref=dst,
        send_sem=send_sem,
        recv_sem=recv_sem,
        device_id={"ep": device},
        device_id_type=MESH,
    )


def place(ep_size):
    me = lax.axis_index("ep")
    return me, me // 4, (me // 2) % 2, me % 2, ep_size // 4


def greet_all(me, ep_size):
    barrier = pltpu.get_barrier_semaphore()
    for step in range(1, ep_size):
        pl.semaphore_signal(
            barrier, inc=1, device_id={"ep": lax.rem(me + step, ep_size)}, device_id_type=MESH
        )
    return barrier


class Gather:
    def __init__(self, ep_size, slots, z_sems, b_sems, c_sems):
        self.me, self.a, self.b, self.c, self.planes = place(ep_size)
        self.slots = slots
        self.z, self.bs, self.cs = z_sems, b_sems, c_sems
        self.sent = []

    def slot(self, core, back, side):
        plane = lax.rem(self.a + (self.planes - back), self.planes)
        return self.slots.at[plane, side, core]

    def device(self, plane, side, core):
        return (plane * 2 + side) * 2 + core

    def along(self, i):
        ref = self.slot(self.c, 0, self.b)
        plane = lax.rem(self.a + i, self.planes)
        return remote(
            ref, ref, self.z.at[0, i], self.z.at[1, i], self.device(plane, self.b, self.c)
        )

    def across(self, i):
        ref = self.slot(self.c, i, self.b)
        return remote(
            ref, ref, self.bs.at[0, i], self.bs.at[1, i], self.device(self.a, 1 - self.b, self.c)
        )

    def to_core(self, kind, i):
        ref = self.slot(self.c, i, self.b if kind == 0 else 1 - self.b)
        return remote(
            ref,
            ref,
            self.cs.at[0, kind, i],
            self.cs.at[1, kind, i],
            self.device(self.a, self.b, 1 - self.c),
        )

    def go(self, copy):
        copy.start()
        self.sent.append(copy)

    def start(self):
        for i in range(1, self.planes):
            self.go(self.along(i))
        self.go(self.across(0))
        self.go(self.to_core(0, 0))

    def arrived(self, ref, sem):
        remote(ref, ref, sem, sem, self.me).wait_recv()

    def relay_side(self, i):
        self.arrived(self.slot(self.c, i, 1 - self.b), self.bs.at[1, i])
        self.go(self.to_core(1, i))

    def relay_plane(self, i):
        self.arrived(self.slot(self.c, i, self.b), self.z.at[1, i])
        self.go(self.across(i))
        self.go(self.to_core(0, i))

    def whole_plane(self, i):
        self.arrived(self.slot(1 - self.c, i, self.b), self.cs.at[1, 0, i])
        self.arrived(self.slot(1 - self.c, i, 1 - self.b), self.cs.at[1, 1, i])

    def drain(self):
        for copy in self.sent:
            copy.wait_send()


def gather_scratch(ep_size, rows, width):
    planes = ep_size // 4
    return [
        pltpu.VMEM((planes, 2, 2, rows, width), BF16),
        pltpu.SemaphoreType.DMA((2, planes)),
        pltpu.SemaphoreType.DMA((2, planes)),
        pltpu.SemaphoreType.DMA((2, 2, planes)),
    ]


def load_all(pairs, sems):
    copies = [pltpu.make_async_copy(src, dst, sems.at[n]) for n, (src, dst) in enumerate(pairs)]
    for copy in copies:
        copy.start()
    return copies


def project_kernel(
    ep_size, experts, hidden_ref, gain_ref, base_ref, routes_ref, gates_ref,
    wr, wk, wv, wdd, wdu, wrd, wru,
    got_ref, decay_ref, removal_ref,
    wdd_v, wdu_v, wrd_v, wru_v, load_sems,
    joint, slots, z_sems, b_sems, c_sems, outbox, inbox, x_send, x_recv,
):
    me, a, b, c, planes = place(ep_size)
    rows, width = hidden_ref.shape
    part = wr.shape[0]
    lanes = joint.shape[0]
    barrier = greet_all(me, ep_size)
    loads = load_all(
        [(wdd, wdd_v), (wrd, wrd_v), (wdu, wdu_v), (wru, wru_v)]
        + [(w, joint.at[pl.ds(n * part, part)]) for n, w in enumerate((wr, wk, wv))],
        load_sems,
    )
    if lanes > 3 * part:
        joint[3 * part :, :] = jnp.zeros((lanes - 3 * part, joint.shape[1]), BF16)
    normed = scaled_rows(hidden_ref[...], gain_ref[...]).astype(BF16)
    slots[a, b, c] = normed
    pl.semaphore_wait(barrier, ep_size - 1)
    gather = Gather(ep_size, slots, z_sems, b_sems, c_sems)
    gather.start()

    for copy in loads[:4]:
        copy.wait()
    decay_low = dot(normed, wdd_v[...]).astype(BF16)
    decay_act = jnp.tanh(decay_low.astype(F32)).astype(BF16)
    decay_pre = base_ref[...] + dot(decay_act, wdu_v[...])
    decay_ref[...] = jnp.exp(-jnp.exp(-jax.nn.softplus(-decay_pre) - 0.5))
    remove_low = dot(normed, wrd_v[...]).astype(BF16)
    removal_ref[...] = jax.nn.sigmoid(dot(remove_low, wru_v[...]))
    for copy in loads[4:]:
        copy.wait()
    lane = lax.broadcasted_iota(jnp.int32, (lanes, rows), 0) - 3 * part
    weight = jnp.zeros((lanes, rows), F32)
    for j in range(routes_ref.shape[0]):
        chosen = routes_ref[j : j + 1, :]
        hit = (lane == chosen) | (lane == chosen + experts)
        weight = weight + jnp.where(hit, gates_ref[j : j + 1, :], 0.0)
    high = weight.astype(BF16).astype(F32)
    spare = jnp.where(lane < experts, high, weight - high)
    spare = jnp.where(lane >= 0, spare, 0.0).astype(BF16)
    same = lax.broadcasted_iota(jnp.int32, (rows, rows), 0) == lax.broadcasted_iota(
        jnp.int32, (rows, rows), 1
    )
    spare = dot_t(same.astype(F32).astype(BF16), spare)

    for i in range(1, planes):
        gather.relay_plane(i)
        gather.relay_side(i - 1)
    gather.relay_side(planes - 1)
    for i in range(planes):
        gather.whole_plane(i)
    rows_all = slots[...].reshape(ep_size * rows, width)
    spread = dot_t(rows_all, joint[...]).reshape(ep_size, rows, lanes)
    outbox[...] = (spread + spare[None]).astype(BF16)
    sends = []
    for step in range(1, ep_size):
        other = lax.rem(me + step, ep_size)
        copy = remote(
            outbox.at[other],
            inbox.at[me],
            x_send.at[step],
            x_recv.at[step],
            other,
        )
        copy.start()
        sends.append(copy)
    inbox[me] = outbox[me]
    for step in range(1, ep_size):
        other = lax.rem(me + (ep_size - step), ep_size)
        ref = inbox.at[other]
        remote(ref, ref, x_recv.at[step], x_recv.at[step], me).wait_recv()
    got_ref[...] = inbox[...]
    gather.drain()
    for copy in sends:
        copy.wait_send()


def mixer_kernel(
    ep_size, hidden_ref, got_ref, decay_ref, removal_ref, ggain_ref, fgain_ref, state_ref, w_out,
    state_out, residual_ref, expert_ref,
    w_out_v, load_sem, recept, keys, values, group, grouped,
):
    step = pl.program_id(0)
    seqs, head, inner = state_ref.shape
    heads = inner // head
    part = inner // ep_size
    load = pltpu.make_async_copy(w_out, w_out_v, load_sem)

    @pl.when(step == 0)
    def _():
        load.start()
        for d in range(ep_size):
            block = got_ref[d].astype(F32)
            own = slice(d * part, (d + 1) * part)
            recept[:, own] = block[:, 0:part]
            keys[:, own] = block[:, part : 2 * part]
            values[:, own] = block[:, 2 * part : 3 * part]
        group[...] = (
            lax.broadcasted_iota(jnp.int32, (inner, heads), 0) // head
            == lax.broadcasted_iota(jnp.int32, (inner, heads), 1)
        ).astype(F32).astype(BF16)

    these = pl.ds(pl.multiple_of(step * seqs, seqs), seqs)
    spread = (
        lax.broadcasted_iota(jnp.int32, (heads, inner), 1) // head
        == lax.broadcasted_iota(jnp.int32, (heads, inner), 0)
    ).astype(F32).astype(BF16)
    own_row = (
        lax.broadcasted_iota(jnp.int32, (head, inner), 1) % head
        == lax.broadcasted_iota(jnp.int32, (head, inner), 0)
    ).astype(F32)
    gather = group[...]
    key = keys[these, :]
    sums = split_dot(key * key, gather)
    unit = key * split_dot(lax.rsqrt(sums + norm_eps), spread)
    removed = unit * removal_ref[these, :]
    recept_now = recept[these, :]
    value_now = values[these, :]
    decay = decay_ref[these, :]
    out_rows = []
    for first in range(0, seqs, MIX):
        ones = [slice(n, n + 1) for n in range(first, first + MIX)]

        def by_row(table):
            return jnp.concatenate(
                [jnp.broadcast_to(table[one], (head, inner)) for one in ones], axis=0
            )

        block = state_ref[first : first + MIX].reshape(MIX * head, inner)
        recalled = dot((block * by_row(unit)).astype(BF16), gather)
        diagonal = jnp.concatenate([own_row * value_now[one] for one in ones], axis=0)
        value_col = dot(diagonal.astype(BF16), gather)
        updated = (
            block * by_row(decay)
            - dot(recalled.astype(BF16), spread) * by_row(removed)
            + dot(value_col.astype(BF16), spread) * by_row(key)
        )
        state_out[first : first + MIX] = updated.reshape(MIX, head, inner)
        readout = dot((updated * by_row(recept_now)).astype(BF16), gather)
        readout = readout.reshape(MIX, head, heads)
        center = readout - jnp.mean(readout, axis=1, keepdims=True)
        var = jnp.mean(center * center, axis=1, keepdims=True)
        normed = (center * lax.rsqrt(var + group_eps)).reshape(MIX * head, heads)
        wide = dot(normed.astype(BF16), spread)
        for n in range(MIX):
            one = wide[n * head : (n + 1) * head] * own_row
            out_rows.append(jnp.sum(one, axis=0, keepdims=True))
    grouped[these, :] = jnp.concatenate(out_rows, axis=0) * ggain_ref[...]

    @pl.when(step == pl.num_programs(0) - 1)
    def _():
        load.wait()
        residual = hidden_ref[...].astype(F32) + dot(grouped[...].astype(BF16), w_out_v[...])
        residual_ref[...] = residual
        expert_ref[...] = scaled_rows(residual, fgain_ref[...]).astype(BF16)


def expert_kernel(
    ep_size, experts, part, expert_ref, residual_ref, got_ref, wg, wu, wd,
    mixed_ref,
    wg_v, wu_v, wd_v, load_sems,
    slots, z_sems, b_sems, c_sems,
    partial, c_out, c_in, c_sem, b_out, b_in, b_sem, z_out, z_in, z_sem,
):
    me, a, b, c, planes = place(ep_size)
    rows, width = expert_ref.shape
    half = planes // 2
    barrier = greet_all(me, ep_size)
    loads = load_all([(wg, wg_v), (wu, wu_v), (wd, wd_v)], load_sems)
    slots[a, b, c] = expert_ref[...]
    pl.semaphore_wait(barrier, ep_size - 1)
    gather = Gather(ep_size, slots, z_sems, b_sems, c_sems)
    gather.start()
    expert = me // EXP_SPLIT
    lane = lax.broadcasted_iota(jnp.int32, got_ref.shape[1:], 1) - 3 * part
    column = (lane == expert) | (lane == expert + experts)
    sends = []

    def back(i):
        return lax.rem(a + (planes - i), planes)

    def send(src, dst, sems, i, device):
        copy = remote(src.at[i], dst.at[i], sems.at[0, i], sems.at[1, i], device)
        copy.start()
        sends.append(copy)

    def landed(dst, sems, i):
        remote(dst.at[i], dst.at[i], sems.at[1, i], sems.at[1, i], me).wait_recv()

    def run(span, after_gate, after_up):
        flat = jnp.concatenate([slots[back(i)].reshape(4 * rows, width) for i in span], axis=0)
        gate_pre = dot_t(flat, wg_v[...])
        after_gate()
        up_pre = dot_t(flat, wu_v[...])
        after_up()
        hidden = (jax.nn.silu(gate_pre) * up_pre).astype(BF16)
        down = dot(hidden, wd_v[...])
        for n, i in enumerate(span):
            weight = jnp.concatenate(
                [
                    jnp.sum(
                        jnp.where(column, got_ref[back(i) * 4 + m].astype(F32), 0.0),
                        axis=-1,
                        keepdims=True,
                    )
                    for m in range(4)
                ],
                axis=0,
            )
            own = down[n * 4 * rows : (n + 1) * 4 * rows] * weight
            partial[i] = own.reshape(2, 2, rows, width)

    def send_core(i):
        c_out[i] = partial[i, :, 1 - c].astype(BF16)
        send(c_out, c_in, c_sem, i, (a * 2 + b) * 2 + 1 - c)

    def send_side(i):
        landed(c_in, c_sem, i)
        b_out[i] = (partial[i, 1 - b, c] + c_in[i, 1 - b].astype(F32)).astype(BF16)
        send(b_out, b_in, b_sem, i, (a * 2 + 1 - b) * 2 + c)

    def joined(i):
        landed(b_in, b_sem, i)
        return partial[i, b, c] + c_in[i, b].astype(F32) + b_in[i].astype(F32)

    def send_plane(i):
        z_out[i] = joined(i).astype(BF16)
        send(z_out, z_in, z_sem, i, (back(i) * 2 + b) * 2 + c)

    first, second = list(range(half)), list(range(half, planes))
    for i in first[1:]:
        gather.relay_plane(i)
    for i in first:
        gather.relay_side(i)
    for i in first:
        gather.whole_plane(i)
    for copy in loads:
        copy.wait()

    def relay(span):
        for i in span:
            gather.relay_plane(i)

    run(first, lambda: relay(second[:1]), lambda: None)
    for i in reversed(first):
        send_core(i)
    relay(second[1:])
    for i in second[:-1]:
        gather.relay_side(i)
    for i in reversed(first):
        send_side(i)
    gather.relay_side(second[-1])
    for i in second:
        gather.whole_plane(i)
    run(second, lambda: None, lambda: [send_plane(i) for i in first[1:]])
    for i in second:
        send_core(i)
    for i in second:
        send_side(i)
    for i in second:
        send_plane(i)
    total = residual_ref[...] + joined(0)
    for i in range(1, planes):
        landed(z_in, z_sem, i)
        total = total + z_in[i].astype(F32)
    mixed_ref[...] = total.astype(BF16)
    gather.drain()
    for copy in sends:
        copy.wait_send()


VM = pl.BlockSpec(memory_space=pltpu.VMEM)
ANY = pl.BlockSpec(memory_space=pl.ANY)
HBM = pl.BlockSpec(memory_space=pltpu.HBM)


def cost(us):
    return pl.CostEstimate(flops=int(us * 2e7), bytes_accessed=2**20, transcendentals=0)


def shards(
    hidden_in, state_in, norm_gain, w_recept, w_key, w_value, decay_base, w_decay_down,
    w_decay_up, w_remove_down, w_remove_up, group_gain, w_out, ffn_gain, routes, route_gate,
    w_gate, w_up, w_down,
):
    ep_size = lax.axis_size("ep")
    experts = ep_size // EXP_SPLIT
    rows, width = hidden_in.shape
    head, inner = state_in.shape[1:]
    part = w_recept.shape[1]
    lanes = -(-(3 * part + 2 * experts) // 128) * 128
    planes = ep_size // 4

    def like(array):
        return pltpu.VMEM(array.shape, array.dtype)

    loaded = (w_decay_down, w_decay_up, w_remove_down, w_remove_up)
    w_gate, w_up = w_gate.T, w_up.T
    got, decay, removal = pl.pallas_call(
        functools.partial(project_kernel, ep_size, experts),
        out_shape=(
            jax.ShapeDtypeStruct((ep_size, rows, lanes), BF16),
            jax.ShapeDtypeStruct((rows, inner), F32),
            jax.ShapeDtypeStruct((rows, inner), F32),
        ),
        in_specs=[VM] * 5 + [HBM] * 7,
        out_specs=(VM, VM, VM),
        scratch_shapes=[like(w) for w in loaded]
        + [pltpu.SemaphoreType.DMA((7,)), pltpu.VMEM((lanes, width), BF16)]
        + gather_scratch(ep_size, rows, width)
        + [
            pltpu.VMEM((ep_size, rows, lanes), BF16),
            pltpu.VMEM((ep_size, rows, lanes), BF16),
            pltpu.SemaphoreType.DMA((ep_size,)),
            pltpu.SemaphoreType.DMA((ep_size,)),
        ],
        compiler_params=pltpu.CompilerParams(
            collective_id=0, has_side_effects=True, vmem_limit_bytes=FULL
        ),
        cost_estimate=cost(20000),
        name="project",
    )(
        hidden_in, norm_gain.reshape(1, -1), decay_base.reshape(1, -1), routes.T, route_gate.T,
        w_recept.T, w_key.T, w_value.T, *loaded
    )

    seqs = min(8, rows)
    whole = lambda *shape: pl.BlockSpec(shape, lambda s: (0,) * len(shape))
    state_spec = pl.BlockSpec((seqs, head, inner), lambda s: (s, 0, 0))
    state_out, residual, expert_in = pl.pallas_call(
        functools.partial(mixer_kernel, ep_size),
        grid=(rows // seqs,),
        out_shape=(
            jax.ShapeDtypeStruct(state_in.shape, F32),
            jax.ShapeDtypeStruct((rows, width), F32),
            jax.ShapeDtypeStruct((rows, width), BF16),
        ),
        in_specs=[
            whole(rows, width),
            whole(ep_size, rows, lanes),
            whole(rows, inner),
            whole(rows, inner),
            whole(1, inner),
            whole(1, width),
            state_spec,
            ANY,
        ],
        out_specs=(state_spec, whole(rows, width), whole(rows, width)),
        scratch_shapes=[
            like(w_out),
            pltpu.SemaphoreType.DMA,
            pltpu.VMEM((rows, inner), F32),
            pltpu.VMEM((rows, inner), F32),
            pltpu.VMEM((rows, inner), F32),
            pltpu.VMEM((inner, inner // head), BF16),
            pltpu.VMEM((rows, inner), F32),
        ],
        compiler_params=pltpu.CompilerParams(
            dimension_semantics=("arbitrary",), vmem_limit_bytes=FULL
        ),
        cost_estimate=cost(10000),
        name="mixer",
    )(
        hidden_in, got, decay, removal, group_gain.reshape(1, -1), ffn_gain.reshape(1, -1),
        state_in, w_out,
    )

    mixed_out = pl.pallas_call(
        functools.partial(expert_kernel, ep_size, experts, part),
        out_shape=jax.ShapeDtypeStruct((rows, width), BF16),
        in_specs=[VM] * 3 + [ANY] * 3,
        out_specs=VM,
        scratch_shapes=[like(w_gate), like(w_up), like(w_down), pltpu.SemaphoreType.DMA((3,))]
        + gather_scratch(ep_size, rows, width)
        + [
            pltpu.VMEM((planes, 2, 2, rows, width), F32),
            pltpu.VMEM((planes, 2, rows, width), BF16),
            pltpu.VMEM((planes, 2, rows, width), BF16),
            pltpu.SemaphoreType.DMA((2, planes)),
            pltpu.VMEM((planes, rows, width), BF16),
            pltpu.VMEM((planes, rows, width), BF16),
            pltpu.SemaphoreType.DMA((2, planes)),
            pltpu.VMEM((planes, rows, width), BF16),
            pltpu.VMEM((planes, rows, width), BF16),
            pltpu.SemaphoreType.DMA((2, planes)),
        ],
        compiler_params=pltpu.CompilerParams(
            collective_id=1, has_side_effects=True, vmem_limit_bytes=FULL
        ),
        cost_estimate=cost(20000),
        name="experts",
    )(expert_in, residual, got, w_gate, w_up, w_down)
    return (mixed_out, state_out)


def solution(mesh):
    placed = (
        P(("grp", "ep"), None),
        P(("grp", "ep"), None, None),
        P(),
        P(None, "ep"),
        P(None, "ep"),
        P(None, "ep"),
        P(),
        P(),
        P(),
        P(),
        P(),
        P(),
        P(),
        P(),
        P(("grp", "ep"), None),
        P(("grp", "ep"), None),
        P(None, "ep"),
        P(None, "ep"),
        P("ep", None),
    )
    return jax.shard_map(
        shards,
        mesh=mesh,
        in_specs=placed,
        out_specs=(P(("grp", "ep"), None), P(("grp", "ep"), None, None)),
        check_vma=False,
    )
```
